32 devices in a mesh: grp: 2 (over x), ep: 16 (over z, y, core).
Axes of the slice: x: 2, y: 2, z: 4, core: 2. Of those that a mesh axis runs over, the one named last changes fastest.
Arguments:
- tokens: bfloat16 [256, 2048], P(('grp', 'ep')), parts along dimension 0, may hold values from -6 to 6
- state: float32 [256, 8, 64, 128], P(('grp', 'ep')), parts along dimension 0, may hold values from -6 to 6
- g_mix: float32 [2048], replicated, may hold values from 0.1 to 1.9
- w_query: bfloat16 [2048, 512], P('ep'), may hold values from -0.125 to 0.125
- w_key: bfloat16 [2048, 512], P('ep'), may hold values from -0.125 to 0.125
- w_value: bfloat16 [2048, 1024], P('ep'), may hold values from -0.125 to 0.125
- w_decay_down: bfloat16 [2048, 32], replicated, may hold values from -0.125 to 0.125
- w_decay_up: bfloat16 [32, 512], replicated, may hold values from -1 to 1
- decay_bias: float32 [512], replicated, may hold values from -6 to 2
- g_head: float32 [128], replicated, may hold values from 0.1 to 1.9
- w_out: bfloat16 [1024, 2048], replicated, may hold values from -0.1875 to 0.1875
- g_ffn: float32 [2048], replicated, may hold values from 0.1 to 1.9
- routes: int32 [256, 4], P(('grp', 'ep')), parts along dimension 0, may hold values from 0 to 31, all different within a row; in each aligned block of 8 rows (0 to 7, 8 to 15, ...) at most 2 rows name the same one
- route_scores: float32 [256, 4], P(('grp', 'ep')), parts along dimension 0, may hold values from -9 to 320
- w_gate_in: bfloat16 [32, 2048, 1024], P('ep'), may hold values from -0.375 to 0.375
- w_lin_in: bfloat16 [32, 2048, 1024], P('ep'), may hold values from -0.375 to 0.375
- w_down: bfloat16 [32, 1024, 2048], P('ep'), may hold values from -0.046875 to 0.046875
Outputs:
- output: bfloat16 [256, 2048], P(('grp', 'ep')), parts along dimension 0
- new_state: float32 [256, 8, 64, 128], P(('grp', 'ep')), parts along dimension 0
The draws below stay inside these ranges and needn't reach their ends.
There are 2 independent parts, one for each index of `grp`. The reference program is written for one: setup_inputs(seed, part) draws one part's arguments, and reference() takes and returns one part's arrays. A program takes and returns all parts, laid end to end along the dimension named above; an argument that names none is the same for every part. Nothing has to cross between parts.
Inputs may be any that keep to these rules, and one draw needn't show every extreme that they name: `routes`: each row names 4 different experts; the rows of one device name no expert more than 2 times, a bound that some block reaches.
All inputs are finite; a program needn't handle non-finite values.
Results may differ from the reference program's by a relative error of at most 0.014.
Values may be sent and summed in bfloat16 or wider, within the bound.
A program may use at most 128 MiB of HBM per device.

```python
import math
import jax
import jax.numpy as jnp
import numpy as np
from jax import lax

D = 2048
HEADS = 8
DK = 64
DV = 128
RANK = 32
FF = 1024
EXPERTS = 32
TOPK = 4
CAP = 2
SEQ_DEV = 8
QK = 512
VW = 1024
TOKENS = 128


def draw_route_scores(key, part):
    base_key = jax.random.fold_in(jax.random.fold_in(key, 11), 0)
    scores = jnp.clip(1.5 * jax.random.normal(base_key, (TOKENS, TOPK), jnp.float32), -9.0, 9.0)
    return scores


def steps_of(rng, extent, shards, low, high):
    def one(dim, parts):
        draws = jax.random.uniform(jax.random.fold_in(jax.random.fold_in(rng, 6), dim), (parts,), jnp.float32, low / len(shards), high / len(shards))
        return jnp.repeat(jnp.exp(draws), extent[dim] // parts).reshape((-1,) + (1,) * (len(extent) - dim - 1))

    loudness = one(*shards[0])
    for cut in shards[1:]:
        loudness = loudness * one(*cut)
    return loudness


def assign_block(stream_key, own, number, rows, count, top, most, slope):
    ranking = jax.random.permutation(stream_key, count)
    crowded, ordinary = portions_of(count, rows * top, most, slope, True), portions_of(count, rows * top, most, slope, False)
    places = jnp.arange(count)

    def named(lengths, turn):
        used = int((lengths > 0).sum())
        fixed = max(1, used // 4)
        shifted = fixed + (places - fixed + turn * (used - fixed)) % max(1, count - fixed)
        return jnp.zeros((count,), jnp.int32).at[ranking[jnp.where(places < fixed, places, shifted)]].set(jnp.asarray(lengths, jnp.int32))

    lengths = jnp.where(number % 4 == 0, named(crowded, number // 4), named(ordinary, number - number // 4 - 1))
    mixed = jax.random.permutation(jax.random.fold_in(own, 3), count)
    donor, sink = mixed[0:count // 2 * 2:2], mixed[1:count // 2 * 2:2]
    room = jnp.minimum(lengths[donor] - 1, most - lengths[sink]) // 2
    room = jnp.where((donor == ranking[0]) | (sink == ranking[0]) | (lengths[sink] == 0), 0, jnp.maximum(room, 0))
    shifted = jax.random.randint(jax.random.fold_in(own, 4), (count // 2,), 0, 1 << 20) % (room + 1)
    lengths = lengths.at[donor].add(-shifted).at[sink].add(shifted)
    items = jnp.searchsorted(jnp.cumsum(lengths), jnp.arange(rows * top), side="right").astype(jnp.int32)
    table = items.reshape(top, rows).T
    table = table[jax.random.permutation(jax.random.fold_in(own, 1), rows)]
    turn = jax.random.randint(jax.random.fold_in(own, 2), (rows, 1), 0, top)
    return jnp.take_along_axis(table, (jnp.arange(top)[None, :] + turn) % top, axis=1)


def portions_of(number_of, total, limit, slope, full):
    loads = [(1 << 20) // math.isqrt(rank ** slope) + 1 for rank in range(1, number_of + 1)]
    largest = limit if full else min(limit, max(-(-total // number_of), total * loads[0] // sum(loads)))
    least = 1 if total - largest >= number_of - 1 else 0
    holding, spare = [largest] + [least] * (number_of - 1), total - largest - least * (number_of - 1)
    while spare > 0:
        movable = [i for i in range(1, number_of) if holding[i] < largest] or [i for i in range(1, number_of) if holding[i] < limit]
        mass, left = sum([loads[i] for i in movable]), spare
        for i in movable:
            addition = min(limit - holding[i], max(1, left * loads[i] // mass), spare)
            holding[i] = holding[i] + addition
            spare = spare - addition
    return np.array(holding)


def centred(own_key, dims, scale, most, pieces=(), held_as=jnp.bfloat16):
    level = steps_of(own_key, dims, pieces, -0.22, 0.18) if pieces else 1.0
    entries = jax.random.normal(own_key, dims, jnp.float32) * scale * level
    return jnp.minimum(jnp.maximum(entries, -most), most).astype(held_as)


def setup_inputs(seed: int = 0, part: int = 0) -> dict:
    key_list = jax.random.split(jax.random.key(seed), 18)
    part_splits = jax.random.split(jax.random.fold_in(key_list[17], part), 18)
    tokens = centred(part_splits[0], (TOKENS, D), 1.0, 6.0, ((0, 16),))
    state = centred(part_splits[1], (TOKENS, HEADS, DK, DV), 1.0, 6.0, ((0, 16),), jnp.float32)
    g_mix = jnp.clip(1.0 + 0.18 * jax.random.normal(key_list[2], (D,), jnp.float32), 0.1, 1.9)
    w_query = centred(key_list[3], (D, QK), D ** -0.5, 0.125, ((0, 16),))
    w_key = centred(key_list[4], (D, QK), D ** -0.5, 0.125, ((0, 16),))
    w_value = centred(key_list[5], (D, VW), D ** -0.5, 0.125, ((0, 16),))
    w_decay_down = centred(key_list[6], (D, RANK), D ** -0.5, 0.125)
    w_decay_up = centred(key_list[7], (RANK, QK), RANK ** -0.5, 1.0)
    decay_bias = jnp.clip(jax.random.uniform(key_list[8], (QK,), jnp.float32, -6.0, 2.0), -6.0, 2.0)
    g_head = jnp.clip(1.0 + 0.18 * jax.random.normal(key_list[9], (DV,), jnp.float32), 0.1, 1.9)
    w_out = centred(key_list[10], (VW, D), VW ** -0.5, 0.1875)
    g_ffn = jnp.clip(1.0 + 0.18 * jax.random.normal(key_list[11], (D,), jnp.float32), 0.1, 1.9)
    routes_keys = jax.random.split(jax.random.fold_in(part_splits[12], 1), TOKENS // SEQ_DEV)
    routes_turns = jax.random.permutation(jax.random.fold_in(part_splits[12], 3), TOKENS // SEQ_DEV)
    routes = jax.vmap(lambda own, number: assign_block(jax.random.fold_in(part_splits[12], 2), own, number, SEQ_DEV, EXPERTS, TOPK, CAP, 2))(routes_keys, routes_turns).reshape((TOKENS, TOPK))
    route_scores = draw_route_scores(jax.random.fold_in(jax.random.fold_in(key_list[17], part), 71), part)
    w_gate_in = centred(key_list[14], (EXPERTS, D, FF), (D // 8) ** -0.5, 0.375, ((0, 16),))
    w_lin_in = centred(key_list[15], (EXPERTS, D, FF), (D // 8) ** -0.5, 0.375, ((0, 16),))
    w_down = centred(key_list[16], (EXPERTS, FF, D), (FF * 16) ** -0.5, 0.046875, ((0, 16),))
    return {"tokens": tokens, "state": state, "g_mix": g_mix, "w_query": w_query, "w_key": w_key, "w_value": w_value, "w_decay_down": w_decay_down, "w_decay_up": w_decay_up, "decay_bias": decay_bias, "g_head": g_head, "w_out": w_out, "g_ffn": g_ffn, "routes": routes, "route_scores": route_scores, "w_gate_in": w_gate_in, "w_lin_in": w_lin_in, "w_down": w_down}


EPS = 1e-06
TAU = 16.0
ALPHA = 1.702
LIMIT = 7.0

def rms_scale(values, gain):
    return values * lax.rsqrt(lax.optimization_barrier(jnp.mean(values * values, axis=-1, keepdims=True)) + EPS) * gain

def expert_apply(fed, gate_weight, lin_weight, down_weight):
    gate_pre = jnp.minimum(jnp.dot(fed, gate_weight, preferred_element_type=jnp.float32), LIMIT)
    lin_pre = jnp.clip(jnp.dot(fed, lin_weight, preferred_element_type=jnp.float32), -LIMIT, LIMIT)
    hidden = (gate_pre * jax.nn.sigmoid(ALPHA * gate_pre) * (lin_pre + 1.0)).astype(jnp.bfloat16)
    return jnp.dot(hidden, down_weight, preferred_element_type=jnp.float32).astype(jnp.bfloat16)

def reference(tokens, state, g_mix, w_query, w_key, w_value, w_decay_down, w_decay_up, decay_bias, g_head, w_out, g_ffn, routes, route_scores, w_gate_in, w_lin_in, w_down):
    seq_rows = tokens.shape[0]
    normed = rms_scale(tokens.astype(jnp.float32), g_mix).astype(jnp.bfloat16)
    queries = jnp.dot(normed, w_query, preferred_element_type=jnp.float32).reshape(seq_rows, HEADS, DK) * DK ** (-0.5)
    key_rows = jnp.dot(normed, w_key, preferred_element_type=jnp.float32).reshape(seq_rows, HEADS, DK)
    value_rows = jnp.dot(normed, w_value, preferred_element_type=jnp.float32).reshape(seq_rows, HEADS, DV)
    low_rank = jnp.dot(normed, w_decay_down, preferred_element_type=jnp.float32).astype(jnp.bfloat16)
    log_decay = jax.nn.log_sigmoid(jnp.dot(low_rank, w_decay_up, preferred_element_type=jnp.float32) + decay_bias) / TAU
    log_decay = log_decay.reshape(seq_rows, HEADS, DK)
    new_state = jnp.exp(log_decay)[..., None] * state + key_rows[..., None] * value_rows[:, :, None, :]
    attended = jnp.einsum('bhk,bhkv->bhv', queries, new_state, precision=lax.Precision.HIGHEST)
    headed = rms_scale(attended, g_head).astype(jnp.bfloat16).reshape(seq_rows, HEADS * DV)
    residual = (tokens.astype(jnp.float32) + jnp.dot(headed, w_out, preferred_element_type=jnp.float32)).astype(jnp.bfloat16)
    fed = rms_scale(residual.astype(jnp.float32), g_ffn).astype(jnp.bfloat16)
    weights = jax.nn.softmax(route_scores, axis=-1)

    def expert_step(expert_index, running):
        chosen = lax.optimization_barrier(jnp.sum(jnp.where(routes == expert_index, weights, jnp.zeros_like(weights)), axis=1))
        expert_out = expert_apply(fed, w_gate_in[expert_index], w_lin_in[expert_index], w_down[expert_index])
        return running + chosen[:, None] * expert_out.astype(jnp.float32)
    expert_sum = lax.fori_loop(0, EXPERTS, expert_step, jnp.zeros((seq_rows, D), jnp.float32))
    output = (residual.astype(jnp.float32) + expert_sum).astype(jnp.bfloat16)
    return (output, new_state)
```

```python
import functools

import jax
import jax.numpy as jnp
from jax import lax
from jax.experimental import pallas as pl
from jax.experimental.pallas import tpu as pltpu
from jax.sharding import PartitionSpec as P

CAP = 2
EPS = 1e-06
TAU = 16.0
ALPHA = 1.702
LIMIT = 7.0
MESH = pl.DeviceIdType.MESH
F32 = jnp.float32
BF16 = jnp.bfloat16


def rms_scale(values, gain):
    return values * lax.rsqrt(jnp.mean(values * values, axis=-1, keepdims=True) + EPS) * gain


def dot(a, b):
    return jnp.dot(a, b, preferred_element_type=F32)


def kernel(
    n,
    tokens_ref,
    g_mix_ref,
    wdd_ref,
    wdu_ref,
    bias_ref,
    g_head_ref,
    g_ffn_ref,
    routes_ref,
    scores_ref,
    state_hbm,
    wq_hbm,
    wk_hbm,
    wv_hbm,
    wo_hbm,
    wg_hbm,
    wl_hbm,
    wd_hbm,
    out_ref,
    new_state_hbm,
    wall,
    st,
    wo,
    wg,
    wl,
    wd,
    nsend,
    nrcv,
    psend,
    prcv,
    q_t,
    k_t,
    d_t,
    v_h,
    att,
    headed,
    xs,
    osend,
    orcv,
    hid,
    rsend,
    rrcv,
    local_sem,
    expert_sem,
    w_sem,
    a_send,
    a_recv,
    b_send,
    b_recv,
    o_send,
    o_recv,
    r_send,
    r_recv,
):
    me = lax.axis_index("ep")
    pairs = n // 2
    core = lax.rem(me, 2)
    pair = me // 2
    sibling = me + 1 - 2 * core
    rows, width = tokens_ref.shape
    _, heads, dk, dv = st.shape
    qk = heads * dk
    local_experts, _, ff = wg.shape
    slots = osend.shape[1]
    pair_k = nsend.shape[2]

    barrier = pltpu.get_barrier_semaphore()
    for d in range(1, n):
        pl.semaphore_signal(
            barrier, inc=1, device_id={"ep": lax.rem(me + d, n)}, device_id_type=MESH
        )
    own = wall.at[core]
    proj = [
        pltpu.make_async_copy(wq_hbm, own.at[:, pl.ds(0, qk)], local_sem.at[0]),
        pltpu.make_async_copy(wk_hbm, own.at[:, pl.ds(qk, qk)], local_sem.at[1]),
        pltpu.make_async_copy(wv_hbm, own.at[:, pl.ds(2 * qk, heads * dv)], local_sem.at[2]),
    ]
    for copy in proj:
        copy.start()
    state_in = pltpu.make_async_copy(state_hbm, st, local_sem.at[3])
    wo_in = pltpu.make_async_copy(wo_hbm, wo, local_sem.at[4])
    state_in.start()
    wo_in.start()

    tokens = tokens_ref[...].astype(F32)
    normed = rms_scale(tokens, g_mix_ref[...]).astype(BF16)
    for j in range(pairs):
        nsend[j] = normed[:, j * pair_k : (j + 1) * pair_k]
    for copy in proj:
        copy.wait()
    pl.semaphore_wait(barrier, n - 1)

    w_copy = pltpu.make_async_remote_copy(
        src_ref=own,
        dst_ref=wall.at[core],
        send_sem=w_sem.at[0],
        recv_sem=w_sem.at[1],
        device_id={"ep": sibling},
        device_id_type=MESH,
    )

    def pair_copies(source, target, send, recv):
        copies = []
        for d in range(1, pairs):
            other = lax.rem(pair + d, pairs)
            copies.append(
                pltpu.make_async_remote_copy(
                    src_ref=source.at[other],
                    dst_ref=target.at[pair],
                    send_sem=send.at[d],
                    recv_sem=recv.at[d],
                    device_id={"ep": other * 2 + core},
                    device_id_type=MESH,
                )
            )
        return copies

    def all_copies(source, target, send, recv):
        copies = []
        for d in range(1, n):
            other = lax.rem(me + d, n)
            copies.append(
                pltpu.make_async_remote_copy(
                    src_ref=source.at[other],
                    dst_ref=target.at[me],
                    send_sem=send.at[d],
                    recv_sem=recv.at[d],
                    device_id={"ep": other},
                    device_id_type=MESH,
                )
            )
        return copies

    a_copies = pair_copies(nsend, nrcv, a_send, a_recv)
    for copy in a_copies:
        copy.start()
    w_copy.start()
    gates, lins, downs = [], [], []
    for e in range(local_experts):
        gates.append(pltpu.make_async_copy(wg_hbm.at[e], wg.at[e], expert_sem.at[0, e]))
        lins.append(pltpu.make_async_copy(wl_hbm.at[e], wl.at[e], expert_sem.at[1, e]))
        downs.append(
            pltpu.make_async_copy(wd_hbm.at[e], wd.at[pl.ds(e * ff, ff)], expert_sem.at[2, e])
        )
    for copy in gates + lins + downs:
        copy.start()

    nrcv[pair] = nsend[pair]
    low_rank = dot(normed, wdd_ref[...]).astype(BF16)
    pre = dot(low_rank, wdu_ref[...]) + bias_ref[...]
    log_decay = (jnp.minimum(pre, 0.0) - jnp.log1p(jnp.exp(-jnp.abs(pre)))) / TAU
    d_t[...] = jnp.transpose(jnp.exp(log_decay))

    routes = routes_ref[...]
    scores = scores_ref[...]
    top = routes.shape[1]
    lanes = max(128, n * slots)
    slot = lax.broadcasted_iota(jnp.int32, (rows, lanes), 1)
    slot_expert = slot // CAP
    slot_rank = slot - slot_expert * CAP
    shifted = jnp.exp(scores - jnp.max(scores, axis=-1, keepdims=True))
    weights = shifted / jnp.sum(shifted, axis=-1, keepdims=True)
    named = jnp.zeros((rows, lanes), F32)
    weighted = jnp.zeros((rows, lanes), F32)
    for k in range(top):
        hit = routes[:, k : k + 1] == slot_expert
        named = named + jnp.where(hit, 1.0, 0.0)
        weighted = weighted + jnp.where(hit, weights[:, k : k + 1], 0.0)
    row_index = lax.broadcasted_iota(jnp.int32, (rows, lanes), 0)
    rank = jnp.zeros((rows, lanes), F32)
    for t in range(rows - 1):
        rank = rank + jnp.where(row_index > t, named[t : t + 1, :], 0.0)
    picked = jnp.where(rank == slot_rank.astype(F32), named, 0.0)
    combine = (weighted * picked)[:, : n * slots]
    combine_high = combine.astype(BF16)
    combine_low = (combine - combine_high.astype(F32)).astype(BF16)
    pick_t = jnp.transpose(picked)[: n * slots, :].astype(BF16)

    w_copy.wait()
    for copy in a_copies:
        copy.wait()
    gathered = nrcv[...].astype(F32).reshape(pairs * rows, pair_k).astype(BF16)
    block = 512
    for j in range(width // block):
        part = dot(
            gathered, wall[:, :, j * block : (j + 1) * block].reshape(pair_k, block)
        )
        psend[:, :, j * block : (j + 1) * block] = part.reshape(pairs, rows, block).astype(BF16)
    b_copies = pair_copies(psend, prcv, b_send, b_recv)
    for copy in b_copies:
        copy.start()
    prcv[pair] = psend[pair]
    for copy in b_copies:
        copy.wait()
    summed = prcv[0].astype(F32)
    for j in range(1, pairs):
        summed = summed + prcv[j].astype(F32)
    q_t[...] = jnp.transpose(summed[:, :qk] * dk ** (-0.5))
    k_t[...] = jnp.transpose(summed[:, qk : 2 * qk])
    for h in range(heads):
        v_h[h] = summed[:, 2 * qk + h * dv : 2 * qk + (h + 1) * dv]
    state_in.wait()

    def head_step(h, carry):
        span = pl.ds(pl.multiple_of(h * dk, dk), dk)
        q_block, k_block, d_block = q_t[span, :], k_t[span, :], d_t[span, :]
        v_block = v_h[h]
        for b in range(rows):
            updated = (
                d_block[:, b : b + 1] * st[b, h] + k_block[:, b : b + 1] * v_block[b : b + 1, :]
            )
            st[b, h] = updated
            att[h, pl.ds(b, 1), :] = jnp.sum(q_block[:, b : b + 1] * updated, axis=0, keepdims=True)
        return carry

    lax.fori_loop(0, heads, head_step, 0)
    state_out = pltpu.make_async_copy(st, new_state_hbm, local_sem.at[5])
    state_out.start()
    for h in range(heads):
        headed[:, h * dv : (h + 1) * dv] = rms_scale(att[h], g_head_ref[...]).astype(BF16)
    wo_in.wait()
    mixed = headed[...]
    residual = jnp.concatenate(
        [dot(mixed, wo[:, j * block : (j + 1) * block]) for j in range(width // block)], axis=1
    )
    residual = (tokens + residual).astype(BF16).astype(F32)
    fed = rms_scale(residual, g_ffn_ref[...]).astype(BF16)
    xs[...] = dot(pick_t, fed)
    for j in range(n):
        osend[j] = xs[j * slots : (j + 1) * slots, :].astype(BF16)
    o_copies = all_copies(osend, orcv, o_send, o_recv)
    for copy in o_copies:
        copy.start()
    orcv[me] = osend[me]
    for copy in o_copies:
        copy.wait()
    for j in range(n):
        xs[j * slots : (j + 1) * slots, :] = orcv[j].astype(F32)

    tile = 256
    row_expert = lax.rem(lax.broadcasted_iota(jnp.int32, (n * slots, tile), 0), slots) // CAP
    x = xs[...].astype(BF16)
    for e in range(local_experts):
        gates[e].wait()
        lins[e].wait()

        def up_step(f, carry, e=e):
            span = pl.ds(pl.multiple_of(f * tile, tile), tile)
            gate = jnp.minimum(dot(x, wg[e, :, span]), LIMIT)
            lin = jnp.clip(dot(x, wl[e, :, span]), -LIMIT, LIMIT)
            value = gate * (1.0 / (1.0 + jnp.exp(-ALPHA * gate))) * (lin + 1.0)
            value = jnp.where(row_expert == e, value, 0.0)
            hid[:, pl.ds(pl.multiple_of(e * ff + f * tile, tile), tile)] = value.astype(BF16)
            return carry

        lax.fori_loop(0, ff // tile, up_step, 0)
    for copy in downs:
        copy.wait()
    hidden = hid[...]

    def down_step(f, carry):
        span = pl.ds(pl.multiple_of(f * tile, tile), tile)
        xs[:, span] = dot(hidden, wd[:, span])
        return carry

    lax.fori_loop(0, width // tile, down_step, 0)
    for j in range(n):
        rsend[j] = xs[j * slots : (j + 1) * slots, :].astype(BF16)
    r_copies = all_copies(rsend, rrcv, r_send, r_recv)
    for copy in r_copies:
        copy.start()
    rrcv[me] = rsend[me]
    for copy in r_copies:
        copy.wait()
    for j in range(n):
        xs[j * slots : (j + 1) * slots, :] = rrcv[j].astype(F32)
    returned = xs[...].astype(BF16)
    expert_sum = dot(combine_high, returned) + dot(combine_low, returned)
    out_ref[...] = (residual + expert_sum).astype(BF16)
    state_out.wait()


def per_device(
    n,
    tokens,
    state,
    g_mix,
    w_query,
    w_key,
    w_value,
    w_decay_down,
    w_decay_up,
    decay_bias,
    g_head,
    w_out,
    g_ffn,
    routes,
    route_scores,
    w_gate_in,
    w_lin_in,
    w_down,
):
    rows, width = tokens.shape
    _, heads, dk, dv = state.shape
    qk = heads * dk
    local_experts, _, ff = w_gate_in.shape
    slots = local_experts * CAP
    pairs = n // 2
    kb = w_query.shape[0]
    vmem = pl.BlockSpec(memory_space=pltpu.VMEM)
    hbm = pl.BlockSpec(memory_space=pl.ANY)
    dma = pltpu.SemaphoreType.DMA
    return pl.pallas_call(
        functools.partial(kernel, n),
        out_shape=(
            jax.ShapeDtypeStruct(tokens.shape, BF16),
            jax.ShapeDtypeStruct(state.shape, F32),
        ),
        in_specs=[vmem] * 9 + [hbm] * 8,
        out_specs=(vmem, hbm),
        scratch_shapes=[
            pltpu.VMEM((2, kb, width), BF16),
            pltpu.VMEM(state.shape, F32),
            pltpu.VMEM(w_out.shape, BF16),
            pltpu.VMEM(w_gate_in.shape, BF16),
            pltpu.VMEM(w_lin_in.shape, BF16),
            pltpu.VMEM((local_experts * ff, width), BF16),
            pltpu.VMEM((pairs, rows, 2 * kb), BF16),
            pltpu.VMEM((pairs, rows, 2 * kb), BF16),
            pltpu.VMEM((pairs, rows, width), BF16),
            pltpu.VMEM((pairs, rows, width), BF16),
            pltpu.VMEM((qk, rows), F32),
            pltpu.VMEM((qk, rows), F32),
            pltpu.VMEM((qk, rows), F32),
            pltpu.VMEM((heads, rows, dv), F32),
            pltpu.VMEM((heads, rows, dv), F32),
            pltpu.VMEM((rows, heads * dv), BF16),
            pltpu.VMEM((n * slots, width), F32),
            pltpu.VMEM((n, slots, width), BF16),
            pltpu.VMEM((n, slots, width), BF16),
            pltpu.VMEM((n * slots, local_experts * ff), BF16),
            pltpu.VMEM((n, slots, width), BF16),
            pltpu.VMEM((n, slots, width), BF16),
            dma((6,)),
            dma((3, local_experts)),
            dma((2,)),
            dma((pairs,)),
            dma((pairs,)),
            dma((pairs,)),
            dma((pairs,)),
            dma((n,)),
            dma((n,)),
            dma((n,)),
            dma((n,)),
        ],
        compiler_params=pltpu.CompilerParams(
            collective_id=0, has_side_effects=True, vmem_limit_bytes=60 * 1024 * 1024
        ),
    )(
        tokens,
        g_mix.reshape(1, -1),
        w_decay_down,
        w_decay_up,
        decay_bias.reshape(1, -1),
        g_head.reshape(1, -1),
        g_ffn.reshape(1, -1),
        routes,
        route_scores,
        state,
        w_query,
        w_key,
        w_value,
        w_out,
        w_gate_in,
        w_lin_in,
        w_down,
    )


def solution(mesh):
    return jax.shard_map(
        functools.partial(per_device, mesh.shape["ep"]),
        mesh=mesh,
        in_specs=(
            P(("grp", "ep"), None),
            P(("grp", "ep"), None, None, None),
            P(),
            P("ep", None),
            P("ep", None),
            P("ep", None),
            P(),
            P(),
            P(),
            P(),
            P(),
            P(),
            P(("grp", "ep"), None),
            P(("grp", "ep"), None),
            P("ep", None, None),
            P("ep", None, None),
            P("ep", None, None),
        ),
        out_specs=(P(("grp", "ep"), None), P(("grp", "ep"), None, None, None)),
        check_vma=False,
    )
```

```python
import functools

import jax
import jax.numpy as jnp
from jax import lax
from jax.experimental import pallas as pl
from jax.experimental.pallas import tpu as pltpu
from jax.sharding import PartitionSpec as P

CAP = 2
EPS = 1e-06
TAU = 16.0
ALPHA = 1.702
LIMIT = 7.0
MESH = pl.DeviceIdType.MESH
F32 = jnp.float32
BF16 = jnp.bfloat16


def rms_scale(values, gain):
    return values * lax.rsqrt(jnp.mean(values * values, axis=-1, keepdims=True) + EPS) * gain


def dot(a, b):
    return jnp.dot(a, b, preferred_element_type=F32)


def kernel(
    n,
    tokens_ref,
    g_mix_ref,
    wdd_ref,
    wdu_ref,
    bias_ref,
    g_head_ref,
    g_ffn_ref,
    routes_ref,
    scores_ref,
    state_hbm,
    wq_hbm,
    wk_hbm,
    wv_hbm,
    wo_hbm,
    wg_hbm,
    wl_hbm,
    wd_hbm,
    out_ref,
    k_t,
    d_t,
    v_h,
    wall,
    st,
    wo,
    wg,
    wl,
    wd,
    nsend,
    nrcv,
    psend,
    prcv,
    q_t,
    att,
    headed,
    xs,
    osend,
    orcv,
    hid,
    rsend,
    rrcv,
    local_sem,
    expert_sem,
    w_sem,
    a_send,
    a_recv,
    b_send,
    b_recv,
    o_send,
    o_recv,
    r_send,
    r_recv,
):
    me = lax.axis_index("ep")
    pairs = n // 2
    core = lax.rem(me, 2)
    pair = me // 2
    sibling = me + 1 - 2 * core
    rows, width = tokens_ref.shape
    _, heads, dk, dv = st.shape
    qk = heads * dk
    local_experts, _, ff = wg.shape
    slots = osend.shape[1]
    pair_k = nsend.shape[2]

    barrier = pltpu.get_barrier_semaphore()
    for d in range(1, n):
        pl.semaphore_signal(
            barrier, inc=1, device_id={"ep": lax.rem(me + d, n)}, device_id_type=MESH
        )
    own = wall.at[core]
    proj = [
        pltpu.make_async_copy(wq_hbm, own.at[:, pl.ds(0, qk)], local_sem.at[0]),
        pltpu.make_async_copy(wk_hbm, own.at[:, pl.ds(qk, qk)], local_sem.at[1]),
        pltpu.make_async_copy(wv_hbm, own.at[:, pl.ds(2 * qk, heads * dv)], local_sem.at[2]),
    ]
    for copy in proj:
        copy.start()
    state_in = pltpu.make_async_copy(state_hbm, st, local_sem.at[3])
    wo_in = pltpu.make_async_copy(wo_hbm, wo, local_sem.at[4])
    state_in.start()
    wo_in.start()

    tokens = tokens_ref[...].astype(F32)
    normed = rms_scale(tokens, g_mix_ref[...]).astype(BF16)
    for j in range(pairs):
        nsend[j] = normed[:, j * pair_k : (j + 1) * pair_k]
    for copy in proj:
        copy.wait()
    pl.semaphore_wait(barrier, n - 1)

    w_copy = pltpu.make_async_remote_copy(
        src_ref=own,
        dst_ref=wall.at[core],
        send_sem=w_sem.at[0],
        recv_sem=w_sem.at[1],
        device_id={"ep": sibling},
        device_id_type=MESH,
    )

    def pair_copies(source, target, send, recv):
        copies = []
        for d in range(1, pairs):
            other = lax.rem(pair + d, pairs)
            copies.append(
                pltpu.make_async_remote_copy(
                    src_ref=source.at[other],
                    dst_ref=target.at[pair],
                    send_sem=send.at[d],
                    recv_sem=recv.at[d],
                    device_id={"ep": other * 2 + core},
                    device_id_type=MESH,
                )
            )
        return copies

    def all_copies(source, target, send, recv):
        copies = []
        for d in range(1, n):
            other = lax.rem(me + d, n)
            copies.append(
                pltpu.make_async_remote_copy(
                    src_ref=source.at[other],
                    dst_ref=target.at[me],
                    send_sem=send.at[d],
                    recv_sem=recv.at[d],
                    device_id={"ep": other},
                    device_id_type=MESH,
                )
            )
        return copies

    a_copies = pair_copies(nsend, nrcv, a_send, a_recv)
    for copy in a_copies:
        copy.start()
    w_copy.start()
    gates, lins, downs = [], [], []
    for e in range(local_experts):
        gates.append(pltpu.make_async_copy(wg_hbm.at[e], wg.at[e], expert_sem.at[0, e]))
        lins.append(pltpu.make_async_copy(wl_hbm.at[e], wl.at[e], expert_sem.at[1, e]))
        downs.append(
            pltpu.make_async_copy(wd_hbm.at[e], wd.at[pl.ds(e * ff, ff)], expert_sem.at[2, e])
        )
    for copy in gates + lins + downs:
        copy.start()

    nrcv[pair] = nsend[pair]
    low_rank = lax.dot_general(
        normed, wdd_ref[...], (((1,), (1,)), ((), ())), preferred_element_type=F32
    ).astype(BF16)
    pre = dot(low_rank, wdu_ref[...]) + bias_ref[...]
    log_decay = (jnp.minimum(pre, 0.0) - jnp.log1p(jnp.exp(-jnp.abs(pre)))) / TAU
    d_t[...] = jnp.transpose(jnp.exp(log_decay))

    routes = routes_ref[...]
    scores = scores_ref[...]
    top = routes.shape[0]
    spots = n * slots
    spot = lax.broadcasted_iota(jnp.int32, (spots, rows), 0)
    spot_expert = spot // CAP
    spot_rank = (spot - spot_expert * CAP).astype(F32)
    shifted = jnp.exp(scores - jnp.max(scores, axis=0, keepdims=True))
    weights = shifted / jnp.sum(shifted, axis=0, keepdims=True)
    named = jnp.zeros((spots, rows), F32)
    weighted = jnp.zeros((spots, rows), F32)
    for k in range(top):
        hit = routes[k : k + 1, :] == spot_expert
        named = named + jnp.where(hit, 1.0, 0.0)
        weighted = weighted + jnp.where(hit, weights[k : k + 1, :], 0.0)
    token = lax.broadcasted_iota(jnp.int32, (spots, rows), 1)
    rank = jnp.zeros((spots, rows), F32)
    for t in range(rows - 1):
        rank = rank + jnp.where(token > t, named[:, t : t + 1], 0.0)
    picked = jnp.where(rank == spot_rank, named, 0.0)
    combine = jnp.transpose(weighted * picked)
    combine_high = combine.astype(BF16)
    combine_low = (combine - combine_high.astype(F32)).astype(BF16)
    pick_t = picked.astype(BF16)

    w_copy.wait()
    for copy in a_copies:
        copy.wait()
    gathered = nrcv[...].astype(F32).reshape(pairs * rows, pair_k).astype(BF16)
    block = 512
    for j in range(width // block):
        part = dot(
            gathered, wall[:, :, j * block : (j + 1) * block].reshape(pair_k, block)
        )
        psend[:, :, j * block : (j + 1) * block] = part.reshape(pairs, rows, block).astype(BF16)
    b_copies = pair_copies(psend, prcv, b_send, b_recv)
    for copy in b_copies:
        copy.start()
    prcv[pair] = psend[pair]
    state_in.wait()

    def decay_step(h, carry):
        d_block = d_t[pl.ds(pl.multiple_of(h * dk, dk), dk), :]
        for b in range(rows):
            st[b, h] = d_block[:, b : b + 1] * st[b, h]
        return carry

    lax.fori_loop(0, heads, decay_step, 0)
    for copy in b_copies:
        copy.wait()
    summed = prcv[0].astype(F32)
    for j in range(1, pairs):
        summed = summed + prcv[j].astype(F32)
    q_t[...] = jnp.transpose(summed[:, :qk] * dk ** (-0.5))
    k_t[...] = jnp.transpose(summed[:, qk : 2 * qk])
    for h in range(heads):
        v_h[h] = summed[:, 2 * qk + h * dv : 2 * qk + (h + 1) * dv]

    def head_step(h, carry):
        q_block = q_t[pl.ds(pl.multiple_of(h * dk, dk), dk), :]
        for b in range(rows):
            att[h, pl.ds(b, 1), :] = jnp.sum(
                q_block[:, b : b + 1] * st[b, h], axis=0, keepdims=True
            )
        return carry

    lax.fori_loop(0, heads, head_step, 0)
    query_key = summed[:, :qk] * dk ** (-0.5) * summed[:, qk : 2 * qk]
    for h in range(heads):
        score = jnp.sum(query_key[:, h * dk : (h + 1) * dk], axis=1, keepdims=True)
        headed[:, h * dv : (h + 1) * dv] = rms_scale(
            att[h] + score * v_h[h], g_head_ref[...]
        ).astype(BF16)
    wo_in.wait()
    mixed = headed[...]
    residual = jnp.concatenate(
        [dot(mixed, wo[:, j * block : (j + 1) * block]) for j in range(width // block)], axis=1
    )
    residual = (tokens + residual).astype(BF16).astype(F32)
    fed = rms_scale(residual, g_ffn_ref[...]).astype(BF16)
    xs[...] = dot(pick_t, fed)
    for j in range(n):
        osend[j] = xs[j * slots : (j + 1) * slots, :].astype(BF16)
    o_copies = all_copies(osend, orcv, o_send, o_recv)
    for copy in o_copies:
        copy.start()
    orcv[me] = osend[me]
    for copy in o_copies:
        copy.wait()
    for j in range(n):
        xs[j * slots : (j + 1) * slots, :] = orcv[j].astype(F32)

    tile = 256
    row_expert = lax.rem(lax.broadcasted_iota(jnp.int32, (n * slots, tile), 0), slots) // CAP
    x = xs[...].astype(BF16)
    for e in range(local_experts):
        gates[e].wait()
        lins[e].wait()

        def up_step(f, carry, e=e):
            span = pl.ds(pl.multiple_of(f * tile, tile), tile)
            gate = jnp.minimum(dot(x, wg[e, :, span]), LIMIT)
            lin = jnp.clip(dot(x, wl[e, :, span]), -LIMIT, LIMIT)
            value = gate * (1.0 / (1.0 + jnp.exp(-ALPHA * gate))) * (lin + 1.0)
            value = jnp.where(row_expert == e, value, 0.0)
            hid[:, pl.ds(pl.multiple_of(e * ff + f * tile, tile), tile)] = value.astype(BF16)
            return carry

        lax.fori_loop(0, ff // tile, up_step, 0)
    for copy in downs:
        copy.wait()
    hidden = hid[...]

    def down_step(f, carry):
        span = pl.ds(pl.multiple_of(f * tile, tile), tile)
        xs[:, span] = dot(hidden, wd[:, span])
        return carry

    lax.fori_loop(0, width // tile, down_step, 0)
    for j in range(n):
        rsend[j] = xs[j * slots : (j + 1) * slots, :].astype(BF16)
    r_copies = all_copies(rsend, rrcv, r_send, r_recv)
    for copy in r_copies:
        copy.start()
    rrcv[me] = rsend[me]
    for copy in r_copies:
        copy.wait()
    for j in range(n):
        xs[j * slots : (j + 1) * slots, :] = rrcv[j].astype(F32)
    returned = xs[...].astype(BF16)
    expert_sum = dot(combine_high, returned) + dot(combine_low, returned)
    out_ref[...] = (residual + expert_sum).astype(BF16)


def finish(layer_ref, k_ref, d_ref, v_ref, state_hbm, out_ref, new_state_hbm, st, in_sem, out_sem):
    rows, heads, dk, _ = st.shape
    ins = [pltpu.make_async_copy(state_hbm.at[b], st.at[b], in_sem.at[b]) for b in range(rows)]
    outs = [pltpu.make_async_copy(st.at[b], new_state_hbm.at[b], out_sem.at[b]) for b in range(rows)]
    for copy in ins:
        copy.start()
    out_ref[...] = layer_ref[...]
    for b in range(rows):
        ins[b].wait()

        def head_step(h, carry, b=b):
            span = pl.ds(pl.multiple_of(h * dk, dk), dk)
            k_block, d_block = k_ref[span, b : b + 1], d_ref[span, b : b + 1]
            st[b, h] = d_block * st[b, h] + k_block * v_ref[h, b : b + 1, :]
            return carry

        lax.fori_loop(0, heads, head_step, 0, unroll=True)
        outs[b].start()
    for copy in outs:
        copy.wait()


def per_device(
    n,
    tokens,
    state,
    g_mix,
    w_query,
    w_key,
    w_value,
    w_decay_down,
    w_decay_up,
    decay_bias,
    g_head,
    w_out,
    g_ffn,
    routes,
    route_scores,
    w_gate_in,
    w_lin_in,
    w_down,
):
    rows, width = tokens.shape
    _, heads, dk, dv = state.shape
    qk = heads * dk
    local_experts, _, ff = w_gate_in.shape
    slots = local_experts * CAP
    pairs = n // 2
    kb = w_query.shape[0]
    vmem = pl.BlockSpec(memory_space=pltpu.VMEM)
    hbm = pl.BlockSpec(memory_space=pl.ANY)
    dma = pltpu.SemaphoreType.DMA
    layer, keys, decays, values = pl.pallas_call(
        functools.partial(kernel, n),
        out_shape=(
            jax.ShapeDtypeStruct(tokens.shape, BF16),
            jax.ShapeDtypeStruct((qk, rows), F32),
            jax.ShapeDtypeStruct((qk, rows), F32),
            jax.ShapeDtypeStruct((heads, rows, dv), F32),
        ),
        in_specs=[vmem] * 9 + [hbm] * 8,
        out_specs=(vmem,) * 4,
        scratch_shapes=[
            pltpu.VMEM((2, kb, width), BF16),
            pltpu.VMEM(state.shape, F32),
            pltpu.VMEM(w_out.shape, BF16),
            pltpu.VMEM(w_gate_in.shape, BF16),
            pltpu.VMEM(w_lin_in.shape, BF16),
            pltpu.VMEM((local_experts * ff, width), BF16),
            pltpu.VMEM((pairs, rows, 2 * kb), BF16),
            pltpu.VMEM((pairs, rows, 2 * kb), BF16),
            pltpu.VMEM((pairs, rows, width), BF16),
            pltpu.VMEM((pairs, rows, width), BF16),
            pltpu.VMEM((qk, rows), F32),
            pltpu.VMEM((heads, rows, dv), F32),
            pltpu.VMEM((rows, heads * dv), BF16),
            pltpu.VMEM((n * slots, width), F32),
            pltpu.VMEM((n, slots, width), BF16),
            pltpu.VMEM((n, slots, width), BF16),
            pltpu.VMEM((n * slots, local_experts * ff), BF16),
            pltpu.VMEM((n, slots, width), BF16),
            pltpu.VMEM((n, slots, width), BF16),
            dma((6,)),
            dma((3, local_experts)),
            dma((2,)),
            dma((pairs,)),
            dma((pairs,)),
            dma((pairs,)),
            dma((pairs,)),
            dma((n,)),
            dma((n,)),
            dma((n,)),
            dma((n,)),
        ],
        compiler_params=pltpu.CompilerParams(
            collective_id=0, has_side_effects=True, vmem_limit_bytes=60 * 1024 * 1024
        ),
    )(
        tokens,
        g_mix.reshape(1, -1),
        w_decay_down.T,
        w_decay_up,
        decay_bias.reshape(1, -1),
        g_head.reshape(1, -1),
        g_ffn.reshape(1, -1),
        routes.T,
        route_scores.T,
        state,
        w_query,
        w_key,
        w_value,
        w_out,
        w_gate_in,
        w_lin_in,
        w_down,
    )
    return pl.pallas_call(
        finish,
        out_shape=(
            jax.ShapeDtypeStruct(tokens.shape, BF16),
            jax.ShapeDtypeStruct(state.shape, F32),
        ),
        in_specs=[vmem] * 4 + [hbm],
        out_specs=(vmem, hbm),
        scratch_shapes=[pltpu.VMEM(state.shape, F32), dma((rows,)), dma((rows,))],
    )(layer, keys, decays, values, state)


def solution(mesh):
    return jax.shard_map(
        functools.partial(per_device, mesh.shape["ep"]),
        mesh=mesh,
        in_specs=(
            P(("grp", "ep"), None),
            P(("grp", "ep"), None, None, None),
            P(),
            P("ep", None),
            P("ep", None),
            P("ep", None),
            P(),
            P(),
            P(),
            P(),
            P(),
            P(),
            P(("grp", "ep"), None),
            P(("grp", "ep"), None),
            P("ep", None, None),
            P("ep", None, None),
            P("ep", None, None),
        ),
        out_specs=(P(("grp", "ep"), None), P(("grp", "ep"), None, None, None)),
        check_vma=False,
    )
```

```python
import functools

import jax
import jax.numpy as jnp
from jax import lax
from jax.experimental import pallas as pl
from jax.experimental.pallas import tpu as pltpu
from jax.sharding import PartitionSpec as P

CAP = 2
EPS = 1e-06
TAU = 16.0
ALPHA = 1.702
LIMIT = 7.0
MESH = pl.DeviceIdType.MESH
F32 = jnp.float32
BF16 = jnp.bfloat16


def rms_scale(values, gain):
    return values * lax.rsqrt(jnp.mean(values * values, axis=-1, keepdims=True) + EPS) * gain


def dot(a, b):
    return jnp.dot(a, b, preferred_element_type=F32)


def kernel(
    n,
    tokens_ref,
    g_mix_ref,
    wdd_ref,
    wdu_ref,
    bias_ref,
    g_head_ref,
    g_ffn_ref,
    routes_ref,
    scores_ref,
    state_hbm,
    wq_hbm,
    wk_hbm,
    wv_hbm,
    wo_hbm,
    wg_hbm,
    wl_hbm,
    wd_hbm,
    out_ref,
    k_ref,
    d_ref,
    v_ref,
    wall,
    st,
    wo,
    wg,
    wl,
    wd,
    nsend,
    nrcv,
    psend,
    prcv,
    st_high,
    st_low,
    att,
    headed,
    xs,
    osend,
    orcv,
    hid,
    rsend,
    rrcv,
    local_sem,
    expert_sem,
    w_sem,
    a_send,
    a_recv,
    b_send,
    b_recv,
    o_send,
    o_recv,
    r_send,
    r_recv,
):
    me = lax.axis_index("ep")
    pairs = n // 2
    core = lax.rem(me, 2)
    pair = me // 2
    sibling = me + 1 - 2 * core
    rows, width = tokens_ref.shape
    _, heads, dk, dv = st.shape
    qk = heads * dk
    local_experts, _, ff = wg.shape
    slots = osend.shape[1]
    pair_k = nsend.shape[2]

    barrier = pltpu.get_barrier_semaphore()
    for d in range(1, n):
        pl.semaphore_signal(
            barrier, inc=1, device_id={"ep": lax.rem(me + d, n)}, device_id_type=MESH
        )
    own = wall.at[core]
    proj = [
        pltpu.make_async_copy(wq_hbm, own.at[:, pl.ds(0, qk)], local_sem.at[0]),
        pltpu.make_async_copy(wk_hbm, own.at[:, pl.ds(qk, qk)], local_sem.at[1]),
        pltpu.make_async_copy(wv_hbm, own.at[:, pl.ds(2 * qk, heads * dv)], local_sem.at[2]),
    ]
    for copy in proj:
        copy.start()
    state_in = pltpu.make_async_copy(state_hbm, st, local_sem.at[3])
    wo_in = pltpu.make_async_copy(wo_hbm, wo, local_sem.at[4])
    state_in.start()
    wo_in.start()

    tokens = tokens_ref[...].astype(F32)
    normed = rms_scale(tokens, g_mix_ref[...]).astype(BF16)
    for j in range(pairs):
        nsend[j] = normed[:, j * pair_k : (j + 1) * pair_k]
    for copy in proj:
        copy.wait()
    pl.semaphore_wait(barrier, n - 1)

    w_copy = pltpu.make_async_remote_copy(
        src_ref=own,
        dst_ref=wall.at[core],
        send_sem=w_sem.at[0],
        recv_sem=w_sem.at[1],
        device_id={"ep": sibling},
        device_id_type=MESH,
    )

    def pair_copies(source, target, send, recv):
        copies = []
        for d in range(1, pairs):
            other = lax.rem(pair + d, pairs)
            copies.append(
                pltpu.make_async_remote_copy(
                    src_ref=source.at[other],
                    dst_ref=target.at[pair],
                    send_sem=send.at[d],
                    recv_sem=recv.at[d],
                    device_id={"ep": other * 2 + core},
                    device_id_type=MESH,
                )
            )
        return copies

    def all_copies(source, target, send, recv):
        copies = []
        for d in range(1, n):
            other = lax.rem(me + d, n)
            copies.append(
                pltpu.make_async_remote_copy(
                    src_ref=source.at[other],
                    dst_ref=target.at[me],
                    send_sem=send.at[d],
                    recv_sem=recv.at[d],
                    device_id={"ep": other},
                    device_id_type=MESH,
                )
            )
        return copies

    a_copies = pair_copies(nsend, nrcv, a_send, a_recv)
    for copy in a_copies:
        copy.start()
    w_copy.start()
    gates, lins, downs = [], [], []
    for e in range(local_experts):
        gates.append(pltpu.make_async_copy(wg_hbm.at[e], wg.at[e], expert_sem.at[0, e]))
        lins.append(pltpu.make_async_copy(wl_hbm.at[e], wl.at[e], expert_sem.at[1, e]))
        downs.append(
            pltpu.make_async_copy(wd_hbm.at[e], wd.at[pl.ds(e * ff, ff)], expert_sem.at[2, e])
        )
    for copy in gates + lins + downs:
        copy.start()

    nrcv[pair] = nsend[pair]
    low_rank = lax.dot_general(
        normed, wdd_ref[...], (((1,), (1,)), ((), ())), preferred_element_type=F32
    ).astype(BF16)
    pre = dot(low_rank, wdu_ref[...]) + bias_ref[...]
    log_decay = (jnp.minimum(pre, 0.0) - jnp.log1p(jnp.exp(-jnp.abs(pre)))) / TAU
    decay = jnp.exp(log_decay)
    d_ref[...] = decay

    routes = routes_ref[...]
    scores = scores_ref[...]
    top = routes.shape[0]
    spots = n * slots
    spot = lax.broadcasted_iota(jnp.int32, (spots, rows), 0)
    spot_expert = spot // CAP
    spot_rank = (spot - spot_expert * CAP).astype(F32)
    shifted = jnp.exp(scores - jnp.max(scores, axis=0, keepdims=True))
    weights = shifted / jnp.sum(shifted, axis=0, keepdims=True)
    named = jnp.zeros((spots, rows), F32)
    weighted = jnp.zeros((spots, rows), F32)
    for k in range(top):
        hit = routes[k : k + 1, :] == spot_expert
        named = named + jnp.where(hit, 1.0, 0.0)
        weighted = weighted + jnp.where(hit, weights[k : k + 1, :], 0.0)
    token = lax.broadcasted_iota(jnp.int32, (spots, rows), 1)
    rank = jnp.zeros((spots, rows), F32)
    for t in range(rows - 1):
        rank = rank + jnp.where(token > t, named[:, t : t + 1], 0.0)
    picked = jnp.where(rank == spot_rank, named, 0.0)
    combine = jnp.transpose(weighted * picked)
    combine_high = combine.astype(BF16)
    combine_low = (combine - combine_high.astype(F32)).astype(BF16)
    pick_t = picked.astype(BF16)

    w_copy.wait()
    for copy in a_copies:
        copy.wait()
    gathered = nrcv[...].astype(F32).reshape(pairs * rows, pair_k).astype(BF16)
    block = 512
    for j in range(width // block):
        part = dot(
            gathered, wall[:, :, j * block : (j + 1) * block].reshape(pair_k, block)
        )
        psend[:, :, j * block : (j + 1) * block] = part.reshape(pairs, rows, block).astype(BF16)
    b_copies = pair_copies(psend, prcv, b_send, b_recv)
    for copy in b_copies:
        copy.start()
    prcv[pair] = psend[pair]
    state_in.wait()

    def split_step(b, carry):
        part = st[b].reshape(qk, dv)
        high = part.astype(BF16)
        st_high[b] = high
        st_low[b] = (part - high.astype(F32)).astype(BF16)
        return carry

    lax.fori_loop(0, rows, split_step, 0)
    for copy in b_copies:
        copy.wait()
    summed = prcv[0].astype(F32)
    for j in range(1, pairs):
        summed = summed + prcv[j].astype(F32)
    queries = summed[:, :qk] * dk ** (-0.5)
    keys = summed[:, qk : 2 * qk]
    k_ref[...] = keys
    v_ref[...] = summed[:, 2 * qk :]
    reads = queries * decay
    head_row = lax.broadcasted_iota(jnp.int32, (heads, qk), 0)
    head_lane = lax.broadcasted_iota(jnp.int32, (heads, qk), 1) // dk
    for b in range(rows):
        spread = jnp.where(head_row == head_lane, reads[b : b + 1, :], 0.0)
        high = spread.astype(BF16)
        low = (spread - high.astype(F32)).astype(BF16)
        read = dot(high, st_high[b]) + (dot(low, st_high[b]) + dot(high, st_low[b]))
        for h in range(heads):
            att[h, b : b + 1, :] = read[h : h + 1, :]
    query_key = queries * keys
    for h in range(heads):
        score = jnp.sum(query_key[:, h * dk : (h + 1) * dk], axis=1, keepdims=True)
        value = summed[:, 2 * qk + h * dv : 2 * qk + (h + 1) * dv]
        headed[:, h * dv : (h + 1) * dv] = rms_scale(
            att[h] + score * value, g_head_ref[...]
        ).astype(BF16)
    wo_in.wait()
    mixed = headed[...]
    residual = jnp.concatenate(
        [dot(mixed, wo[:, j * block : (j + 1) * block]) for j in range(width // block)], axis=1
    )
    residual = (tokens + residual).astype(BF16).astype(F32)
    fed = rms_scale(residual, g_ffn_ref[...]).astype(BF16)
    xs[...] = dot(pick_t, fed)
    for j in range(n):
        osend[j] = xs[j * slots : (j + 1) * slots, :].astype(BF16)
    o_copies = all_copies(osend, orcv, o_send, o_recv)
    for copy in o_copies:
        copy.start()
    orcv[me] = osend[me]
    for copy in o_copies:
        copy.wait()
    for j in range(n):
        xs[j * slots : (j + 1) * slots, :] = orcv[j].astype(F32)

    tile = 256
    row_expert = lax.rem(lax.broadcasted_iota(jnp.int32, (n * slots, tile), 0), slots) // CAP
    x = xs[...].astype(BF16)
    for e in range(local_experts):
        gates[e].wait()
        lins[e].wait()

        def up_step(f, carry, e=e):
            span = pl.ds(pl.multiple_of(f * tile, tile), tile)
            gate = jnp.minimum(dot(x, wg[e, :, span]), LIMIT)
            lin = jnp.clip(dot(x, wl[e, :, span]), -LIMIT, LIMIT)
            value = gate * (1.0 / (1.0 + jnp.exp(-ALPHA * gate))) * (lin + 1.0)
            value = jnp.where(row_expert == e, value, 0.0)
            hid[:, pl.ds(pl.multiple_of(e * ff + f * tile, tile), tile)] = value.astype(BF16)
            return carry

        lax.fori_loop(0, ff // tile, up_step, 0)
    for copy in downs:
        copy.wait()
    hidden = hid[...]

    def down_step(f, carry):
        span = pl.ds(pl.multiple_of(f * tile, tile), tile)
        xs[:, span] = dot(hidden, wd[:, span])
        return carry

    half = width // 2
    r_copies = []
    for part in range(2):
        steps = half // tile
        lax.fori_loop(part * steps, (part + 1) * steps, down_step, 0)
        for j in range(n):
            rsend[part, j] = xs[
                j * slots : (j + 1) * slots, part * half : (part + 1) * half
            ].astype(BF16)
        copies = all_copies(rsend.at[part], rrcv.at[part], r_send.at[part], r_recv.at[part])
        for copy in copies:
            copy.start()
        rrcv[part, me] = rsend[part, me]
        r_copies.append(copies)
    for part in range(2):
        for copy in r_copies[part]:
            copy.wait()
        for j in range(n):
            xs[j * slots : (j + 1) * slots, part * half : (part + 1) * half] = rrcv[
                part, j
            ].astype(F32)
    returned = xs[...].astype(BF16)
    expert_sum = dot(combine_high, returned) + dot(combine_low, returned)
    out_ref[...] = (residual + expert_sum).astype(BF16)


def finish(layer_ref, k_ref, d_ref, v_ref, state_hbm, out_ref, new_state_hbm, st, in_sem, out_sem):
    rows, heads, dk, dv = st.shape
    ins = [pltpu.make_async_copy(state_hbm.at[b], st.at[b], in_sem.at[b]) for b in range(rows)]
    outs = [pltpu.make_async_copy(st.at[b], new_state_hbm.at[b], out_sem.at[b]) for b in range(rows)]
    for copy in ins:
        copy.start()
    out_ref[...] = layer_ref[...]
    parts = []
    for ref in (d_ref, k_ref):
        high = ref[...].astype(BF16).astype(F32)
        parts += [high, ref[...] - high]
    columns = jnp.transpose(jnp.concatenate(parts, axis=0)).astype(BF16)
    shape = (4 * rows, 2 * dv)
    part_row = lax.broadcasted_iota(jnp.int32, shape, 0)
    same_kind = (part_row < 2 * rows) == (lax.broadcasted_iota(jnp.int32, shape, 1) < dv)
    for b in range(rows):
        chosen = same_kind & (lax.rem(part_row, rows) == b)
        spread = dot(columns, jnp.where(chosen, 1.0, 0.0).astype(BF16))
        ins[b].wait()
        for h in range(heads):
            span = slice(h * dk, (h + 1) * dk)
            value = v_ref[b : b + 1, h * dv : (h + 1) * dv]
            st[b, h] = spread[span, :dv] * st[b, h] + spread[span, dv:] * value
        outs[b].start()
    for copy in outs:
        copy.wait()


def per_device(
    n,
    tokens,
    state,
    g_mix,
    w_query,
    w_key,
    w_value,
    w_decay_down,
    w_decay_up,
    decay_bias,
    g_head,
    w_out,
    g_ffn,
    routes,
    route_scores,
    w_gate_in,
    w_lin_in,
    w_down,
):
    rows, width = tokens.shape
    _, heads, dk, dv = state.shape
    qk = heads * dk
    local_experts, _, ff = w_gate_in.shape
    slots = local_experts * CAP
    pairs = n // 2
    kb = w_query.shape[0]
    vmem = pl.BlockSpec(memory_space=pltpu.VMEM)
    hbm = pl.BlockSpec(memory_space=pl.ANY)
    dma = pltpu.SemaphoreType.DMA
    layer, keys, decays, values = pl.pallas_call(
        functools.partial(kernel, n),
        out_shape=(
            jax.ShapeDtypeStruct(tokens.shape, BF16),
            jax.ShapeDtypeStruct((rows, qk), F32),
            jax.ShapeDtypeStruct((rows, qk), F32),
            jax.ShapeDtypeStruct((rows, heads * dv), F32),
        ),
        in_specs=[vmem] * 9 + [hbm] * 8,
        out_specs=(vmem,) * 4,
        scratch_shapes=[
            pltpu.VMEM((2, kb, width), BF16),
            pltpu.VMEM(state.shape, F32),
            pltpu.VMEM(w_out.shape, BF16),
            pltpu.VMEM(w_gate_in.shape, BF16),
            pltpu.VMEM(w_lin_in.shape, BF16),
            pltpu.VMEM((local_experts * ff, width), BF16),
            pltpu.VMEM((pairs, rows, 2 * kb), BF16),
            pltpu.VMEM((pairs, rows, 2 * kb), BF16),
            pltpu.VMEM((pairs, rows, width), BF16),
            pltpu.VMEM((pairs, rows, width), BF16),
            pltpu.VMEM((rows, qk, dv), BF16),
            pltpu.VMEM((rows, qk, dv), BF16),
            pltpu.VMEM((heads, rows, dv), F32),
            pltpu.VMEM((rows, heads * dv), BF16),
            pltpu.VMEM((n * slots, width), F32),
            pltpu.VMEM((n, slots, width), BF16),
            pltpu.VMEM((n, slots, width), BF16),
            pltpu.VMEM((n * slots, local_experts * ff), BF16),
            pltpu.VMEM((2, n, slots, width // 2), BF16),
            pltpu.VMEM((2, n, slots, width // 2), BF16),
            dma((6,)),
            dma((3, local_experts)),
            dma((2,)),
            dma((pairs,)),
            dma((pairs,)),
            dma((pairs,)),
            dma((pairs,)),
            dma((n,)),
            dma((n,)),
            dma((2, n)),
            dma((2, n)),
        ],
        compiler_params=pltpu.CompilerParams(
            collective_id=0, has_side_effects=True, vmem_limit_bytes=60 * 1024 * 1024
        ),
    )(
        tokens,
        g_mix.reshape(1, -1),
        w_decay_down.T,
        w_decay_up,
        decay_bias.reshape(1, -1),
        g_head.reshape(1, -1),
        g_ffn.reshape(1, -1),
        routes.T,
        route_scores.T,
        state,
        w_query,
        w_key,
        w_value,
        w_out,
        w_gate_in,
        w_lin_in,
        w_down,
    )
    return pl.pallas_call(
        finish,
        out_shape=(
            jax.ShapeDtypeStruct(tokens.shape, BF16),
            jax.ShapeDtypeStruct(state.shape, F32),
        ),
        in_specs=[vmem] * 4 + [hbm],
        out_specs=(vmem, hbm),
        scratch_shapes=[pltpu.VMEM(state.shape, F32), dma((rows,)), dma((rows,))],
    )(layer, keys, decays, values, state)


def solution(mesh):
    return jax.shard_map(
        functools.partial(per_device, mesh.shape["ep"]),
        mesh=mesh,
        in_specs=(
            P(("grp", "ep"), None),
            P(("grp", "ep"), None, None, None),
            P(),
            P("ep", None),
            P("ep", None),
            P("ep", None),
            P(),
            P(),
            P(),
            P(),
            P(),
            P(),
            P(("grp", "ep"), None),
            P(("grp", "ep"), None),
            P("ep", None, None),
            P("ep", None, None),
            P("ep", None, None),
        ),
        out_specs=(P(("grp", "ep"), None), P(("grp", "ep"), None, None, None)),
        check_vma=False,
    )
```
